128 devices in a mesh: ra: 16 (over z, x), cb: 8 (over y, core).
Axes of the slice: x: 4, y: 4, z: 4, core: 2. Of those that a mesh axis runs over, the one named last changes fastest.
Arguments:
- stream: bfloat16 [128, 2048], P(None, 'ra'), may hold values from -6 to 6
- gain_first: float32 [2048], P('ra'), may hold values from 0.5 to 1.5
- lift_first: bfloat16 [2048, 8192], P('ra', 'cb'), may hold values from -0.125 to 0.125
- drop_first: bfloat16 [8192, 2048], P('cb', 'ra'), may hold values from -0.0625 to 0.0625
- gain_second: float32 [2048], P('ra'), may hold values from 0.5 to 1.5
- lift_second: bfloat16 [2048, 8192], P('ra', 'cb'), may hold values from -0.125 to 0.125
- drop_second: bfloat16 [8192, 2048], P('cb', 'ra'), may hold values from -0.0625 to 0.0625
Outputs:
- stream_out: bfloat16 [128, 2048], P(None, 'ra')
The draws below stay inside these ranges and needn't reach their ends.
All inputs are finite; a program needn't handle non-finite values.
Results may differ from the reference program's by a relative error of at most 0.0075.
Values may be sent and summed in bfloat16 or wider, within the bound.
A program may use at most 64 MiB of HBM per device.

```python
import jax
import jax.numpy as jnp
from jax import lax

D = 2048
HIDDEN_SIZE = 8192
TOKENS = 128


def level_of(own_key, extent, split, low, largest):
    loudness, own = 1.0, jax.random.fold_in(own_key, 6)
    for dim, blocks in split:
        draws = jnp.exp(jax.random.uniform(jax.random.fold_in(own, dim), (blocks,), jnp.float32, low / len(split), largest / len(split)))
        loudness = loudness * jnp.repeat(draws, extent[dim] // blocks).reshape([-1 if axis == dim else 1 for axis in range(len(extent))])
    return loudness


def noise(stream_key, shape, width, bound, cuts=(), kind=jnp.bfloat16):
    array = jax.random.normal(stream_key, shape, jnp.float32) * width
    if len(cuts) > 0:
        array = level_of(stream_key, shape, cuts, -0.22, 0.18) * array
    return jnp.clip(array, min=-bound, max=bound).astype(kind)


def setup_inputs(seed: int = 0) -> dict:
    seeds = jax.random.split(jax.random.key(seed), 8)
    return {
        "stream": noise(seeds[0], (TOKENS, D), 1.0, 6.0, ((1, 16),)),
        "gain_first": jnp.clip(1.0 + 0.1 * jax.random.normal(seeds[1], (D,), jnp.float32), 0.5, 1.5),
        "lift_first": noise(seeds[2], (D, HIDDEN_SIZE), D ** -0.5, 0.125, ((0, 16), (1, 8))),
        "drop_first": noise(seeds[3], (HIDDEN_SIZE, D), HIDDEN_SIZE ** -0.5, 0.0625, ((0, 8), (1, 16))),
        "gain_second": jnp.clip(1.0 + 0.1 * jax.random.normal(seeds[4], (D,), jnp.float32), 0.5, 1.5),
        "lift_second": noise(seeds[5], (D, HIDDEN_SIZE), D ** -0.5, 0.125, ((0, 16), (1, 8))),
        "drop_second": noise(seeds[6], (HIDDEN_SIZE, D), HIDDEN_SIZE ** -0.5, 0.0625, ((0, 8), (1, 16))),
    }


residual_scale = 0.25
epsilon = 1e-6


def sublayer(stream, gain_vector, lift_weight, drop_weight):
    feature_count = stream.shape[-1]
    widened = stream.astype(jnp.float32)
    squares = jnp.sum(widened * widened, axis=-1, keepdims=True)
    gained = (widened * gain_vector.astype(jnp.float32)).astype(jnp.bfloat16)
    pre_act = jnp.dot(gained, lift_weight, preferred_element_type=jnp.float32)
    pre_act = pre_act * lax.rsqrt(squares / feature_count + epsilon)
    hidden = jnp.square(jnp.maximum(pre_act, 0.0)).astype(jnp.bfloat16)
    branch = jnp.dot(hidden, drop_weight, preferred_element_type=jnp.float32)
    return (residual_scale * widened + branch).astype(jnp.bfloat16)


def reference(stream, gain_first, lift_first, drop_first, gain_second, lift_second, drop_second):
    middle = sublayer(stream, gain_first, lift_first, drop_first)
    return sublayer(middle, gain_second, lift_second, drop_second)
```

```python
import functools

import jax
import jax.numpy as jnp
from jax import lax
from jax.experimental import pallas as pl
from jax.experimental.pallas import tpu as pltpu
from jax.sharding import PartitionSpec as P

MESH = pl.DeviceIdType.MESH
F32 = jnp.float32
BF16 = jnp.bfloat16

residual_scale = 0.25
epsilon = 1e-06

SIDE = 4
RA = SIDE * SIDE
FEATURES = 2048

OFFSETS = sorted(
    [(dz, dx) for dz in range(SIDE) for dx in range(SIDE) if (dz, dx) != (0, 0)],
    key=lambda o: -(min(o[0], SIDE - o[0]) + min(o[1], SIDE - o[1])),
)


def kernel(
    stream_hbm, gain1_hbm, lift1_hbm, drop1_hbm, gain2_hbm, lift2_hbm, drop2_hbm, out_ref,
    stream, gain, lift, drop, part, part_in, hid, branch, branch_in, pair, pair_in, sq, sq_in,
    load_sem, part_ssem, part_rsem, hid_ssem, hid_rsem, br_ssem, br_rsem, pair_ssem, pair_rsem, sq_ssem, sq_rsem,
):
    ra = lax.axis_index("ra")
    cb = lax.axis_index("cb")
    z, x = ra // SIDE, ra % SIDE
    y, core = cb // 2, cb % 2
    half = part.shape[2]

    loads = [
        pltpu.make_async_copy(src, dst, load_sem.at[i])
        for i, (src, dst) in enumerate([
            (stream_hbm, stream), (gain1_hbm, gain.at[0]), (lift1_hbm, lift.at[0]), (drop1_hbm, drop.at[0]),
            (gain2_hbm, gain.at[1]), (lift2_hbm, lift.at[1]), (drop2_hbm, drop.at[1]),
        ])
    ]
    for load in loads:
        load.start()

    peers = [lax.rem(z + dz, SIDE) * SIDE + lax.rem(x + dx, SIDE) for dz, dx in OFFSETS]
    columns = [lax.rem(y + dy, SIDE) * 2 + core for dy in (2, 1, 3)]
    partner = cb + 1 - 2 * core

    barrier = pltpu.get_barrier_semaphore()
    for peer in peers:
        pl.semaphore_signal(barrier, inc=1, device_id=(peer, cb), device_id_type=MESH)
    for column in columns:
        pl.semaphore_signal(barrier, inc=1, device_id=(ra, column), device_id_type=MESH)
    pl.semaphore_signal(barrier, inc=1, device_id=(ra, partner), device_id_type=MESH)

    pending = []

    def send(src, dst, ssem, rsem, device):
        copy = pltpu.make_async_remote_copy(
            src_ref=src, dst_ref=dst, send_sem=ssem, recv_sem=rsem, device_id=device, device_id_type=MESH
        )
        copy.start()
        pending.append(copy)

    def arrive(dst, ssem, rsem):
        pltpu.make_async_remote_copy(
            src_ref=dst, dst_ref=dst, send_sem=ssem, recv_sem=rsem, device_id=(ra, cb), device_id_type=MESH
        ).wait_recv()

    loads[0].wait()
    loads[1].wait()
    current = stream[...].astype(F32)
    for layer in range(2):
        if layer == 1:
            loads[4].wait()
        gained = (current * gain[layer]).astype(BF16)
        squares = current * current
        sq[layer] = jnp.sum(squares.T, axis=0, keepdims=True)
        loads[2 + 3 * layer].wait()
        products = jnp.dot(gained, lift[layer], preferred_element_type=F32)
        for i in range(RA):
            rows, cols = i // 8, i % 8
            part[layer, i] = products[rows * half:(rows + 1) * half, cols * 128:(cols + 1) * 128].astype(BF16)
        if layer == 0:
            pl.semaphore_wait(barrier, RA - 1 + SIDE)
        for k, peer in enumerate(peers):
            send(part.at[layer, peer], part_in.at[layer, ra], part_ssem.at[layer, k], part_rsem.at[layer, ra], (peer, cb))
        for k, peer in enumerate(peers):
            send(sq.at[layer], sq_in.at[layer, ra], sq_ssem.at[layer, k], sq_rsem.at[layer, ra], (peer, cb))

        total = part[layer, ra].astype(F32)
        for k in reversed(range(RA - 1)):
            peer = peers[k]
            arrive(part_in.at[layer, peer], part_ssem.at[layer, k], part_rsem.at[layer, peer])
            total += part_in[layer, peer].astype(F32)
        positive = jnp.maximum(total, 0.0)
        hid[layer, ra] = (positive * positive).astype(BF16)
        for k, peer in enumerate(peers):
            send(hid.at[layer, ra], hid.at[layer, ra], hid_ssem.at[layer, k], hid_rsem.at[layer, ra], (peer, cb))

        sq_in[layer, ra] = sq[layer]
        for k in range(RA - 1):
            arrive(sq_in.at[layer, peers[k]], sq_ssem.at[layer, k], sq_rsem.at[layer, peers[k]])
        sums = sq_in[layer, 0]
        for i in range(1, RA):
            sums += sq_in[layer, i]
        scale = jnp.broadcast_to(1.0 / (sums / FEATURES + epsilon), (128, 128)).T

        loads[3 + 3 * layer].wait()
        for k in reversed(range(RA - 1)):
            peer = peers[k]
            arrive(hid.at[layer, peer], hid_ssem.at[layer, k], hid_rsem.at[layer, peer])
        for rows in range(2):
            hidden = jnp.concatenate([hid[layer, rows * 8 + i] for i in range(8)], axis=1)
            mine = jnp.dot(hidden, drop[layer], preferred_element_type=F32)
            branch[layer, rows * half:(rows + 1) * half] = mine.astype(BF16)
        for k, column in enumerate(columns):
            send(branch.at[layer], branch_in.at[layer, y], br_ssem.at[layer, k], br_rsem.at[layer, y], (ra, column))
        branch_in[layer, y] = branch[layer]
        for k, column in reversed(list(enumerate(columns))):
            arrive(branch_in.at[layer, column // 2], br_ssem.at[layer, k], br_rsem.at[layer, column // 2])
        summed = branch_in[layer, 0].astype(F32)
        for i in range(1, SIDE):
            summed += branch_in[layer, i].astype(F32)
        pair[layer] = summed
        send(pair.at[layer], pair_in.at[layer], pair_ssem.at[layer], pair_rsem.at[layer], (ra, partner))
        arrive(pair_in.at[layer], pair_ssem.at[layer], pair_rsem.at[layer])
        after = (residual_scale * current + scale * (summed + pair_in[layer])).astype(BF16)
        current = after.astype(F32)

    out_ref[...] = after
    for copy in pending:
        copy.wait_send()


def per_device(stream, gain_first, lift_first, drop_first, gain_second, lift_second, drop_second):
    tokens, width = stream.shape
    hidden = lift_first.shape[1]
    any_spec = pl.BlockSpec(memory_space=pl.ANY)
    dma = pltpu.SemaphoreType.DMA
    return pl.pallas_call(
        kernel,
        out_shape=jax.ShapeDtypeStruct((tokens, width), BF16),
        in_specs=[any_spec] * 7,
        out_specs=pl.BlockSpec(memory_space=pltpu.VMEM),
        scratch_shapes=[
            pltpu.VMEM((tokens, width), BF16),
            pltpu.VMEM((2, 1, width), F32),
            pltpu.VMEM((2, width, hidden), BF16),
            pltpu.VMEM((2, hidden, width), BF16),
            pltpu.VMEM((2, RA, tokens // 2, 128), BF16),
            pltpu.VMEM((2, RA, tokens // 2, 128), BF16),
            pltpu.VMEM((2, RA, tokens // 2, 128), BF16),
            pltpu.VMEM((2, tokens, width), BF16),
            pltpu.VMEM((2, SIDE, tokens, width), BF16),
            pltpu.VMEM((2, tokens, width), F32),
            pltpu.VMEM((2, tokens, width), F32),
            pltpu.VMEM((2, 1, tokens), F32),
            pltpu.VMEM((2, RA, 1, tokens), F32),
            dma((7,)),
            dma((2, RA)), dma((2, RA)),
            dma((2, RA)), dma((2, RA)),
            dma((2, SIDE)), dma((2, SIDE)),
            dma((2,)), dma((2,)),
            dma((2, RA)), dma((2, RA)),
        ],
        compiler_params=pltpu.CompilerParams(collective_id=0, has_side_effects=True),
        name="ffn_pair",
    )(
        stream, gain_first.reshape(1, width), lift_first, drop_first,
        gain_second.reshape(1, width), lift_second, drop_second,
    )


def solution(mesh):
    in_specs = (P(None, "ra"), P("ra"), P("ra", "cb"), P("cb", "ra"), P("ra"), P("ra", "cb"), P("cb", "ra"))
    return jax.shard_map(
        per_device, mesh=mesh, in_specs=in_specs, out_specs=P(None, "ra"), check_vma=False
    )
```

```python
import jax
import jax.numpy as jnp
from jax import lax
from jax.experimental import pallas as pl
from jax.experimental.pallas import tpu as pltpu
from jax.sharding import PartitionSpec as P

MESH = pl.DeviceIdType.MESH
F32 = jnp.float32
BF16 = jnp.bfloat16

residual_scale = 0.25
epsilon = 1e-06

SIDE = 4
RA = SIDE * SIDE
CB = 2 * SIDE
FEATURES = 2048
LANES = 128
BLOCKS = 2
SPLIT = 2
GROUPS = RA // SPLIT

OFFSETS = sorted(
    [(dz, dx) for dz in range(SIDE) for dx in range(SIDE) if (dz, dx) != (0, 0)],
    key=lambda o: -(min(o[0], SIDE - o[0]) + min(o[1], SIDE - o[1])),
)
COLUMN_OFFSETS = [(2, 0), (2, 1), (1, 0), (1, 1), (3, 0), (3, 1), (0, 1)]


def kernel(
    stream_hbm, gain1_hbm, lift1_hbm, drop1_hbm, gain2_hbm, lift2_hbm, drop2_hbm, out_ref,
    stream, gain, lift, drop, part, part_in, hid, branch, sq, sq_in,
    load_sem, part_ssem, part_rsem, hid_ssem, hid_rsem, br_ssem, br_rsem, sq_ssem, sq_rsem,
):
    ra = lax.axis_index("ra")
    cb = lax.axis_index("cb")
    z, x = ra // SIDE, ra % SIDE
    y, core = cb // 2, cb % 2
    tokens = stream.shape[0]
    size = tokens // BLOCKS
    rows = size // SPLIT

    peers = [lax.rem(z + dz, SIDE) * SIDE + lax.rem(x + dx, SIDE) for dz, dx in OFFSETS]
    columns = [lax.rem(y + dy, SIDE) * 2 + lax.rem(core + dc, 2) for dy, dc in COLUMN_OFFSETS]

    barrier = pltpu.get_barrier_semaphore()
    for peer in peers:
        pl.semaphore_signal(barrier, inc=1, device_id=(peer, cb), device_id_type=MESH)
    for column in columns:
        pl.semaphore_signal(barrier, inc=1, device_id=(ra, column), device_id_type=MESH)

    loads = [
        pltpu.make_async_copy(src, dst, load_sem.at[i])
        for i, (src, dst) in enumerate([
            (stream_hbm, stream), (gain1_hbm, gain.at[0]), (lift1_hbm, lift.at[0]), (drop1_hbm, drop.at[0]),
            (gain2_hbm, gain.at[1]), (lift2_hbm, lift.at[1]), (drop2_hbm, drop.at[1]),
        ])
    ]
    for load in loads:
        load.start()

    def send(src, dst, ssem, rsem, device):
        pltpu.make_async_remote_copy(
            src_ref=src, dst_ref=dst, send_sem=ssem, recv_sem=rsem, device_id=device, device_id_type=MESH
        ).start()

    def arrived(ref, rsem):
        pltpu.make_async_copy(ref, ref, rsem).wait()

    def multiply_in(layer, b, current):
        gained = (current * gain[layer]).astype(BF16)
        products = jnp.dot(gained, lift[layer], preferred_element_type=F32).astype(BF16)
        for i in range(RA):
            r, c = i // GROUPS, i % GROUPS
            part[layer, b, i] = products[r * rows:(r + 1) * rows, c * LANES:(c + 1) * LANES]

    def scatter(layer, b):
        for k, peer in enumerate(peers):
            send(part.at[layer, b, peer], part_in.at[layer, b, k], part_ssem.at[layer, b], part_rsem.at[layer, b], (peer, cb))

    def send_squares(layer, current):
        sq[layer] = jnp.sum((current * current).T, axis=0, keepdims=True)
        for k, peer in enumerate(peers):
            send(sq.at[layer], sq_in.at[layer, k], sq_ssem.at[layer], sq_rsem.at[layer], (peer, cb))

    def activate(layer, b):
        arrived(part_in.at[layer, b], part_rsem.at[layer, b])
        total = part[layer, b, ra].astype(F32)
        for k in range(RA - 1):
            total += part_in[layer, b, k].astype(F32)
        positive = jnp.maximum(total, 0.0)
        hid[layer, b, ra] = (positive * positive).astype(BF16)
        for peer in peers:
            send(hid.at[layer, b, ra], hid.at[layer, b, ra], hid_ssem.at[layer, b], hid_rsem.at[layer, b], (peer, cb))

    def token_scale(layer):
        arrived(sq_in.at[layer], sq_rsem.at[layer])
        sums = sq[layer]
        for k in range(RA - 1):
            sums += sq_in[layer, k]
        return jnp.broadcast_to(1.0 / (sums / FEATURES + epsilon), (tokens, tokens)).T

    def multiply_out(layer, b):
        arrived(hid.at[layer, b, pl.ds(0, RA - 1)], hid_rsem.at[layer, b])
        hidden = jnp.concatenate([
            jnp.concatenate([hid[layer, b, r * GROUPS + c] for c in range(GROUPS)], axis=1) for r in range(SPLIT)
        ], axis=0)
        branch[layer, b, cb] = jnp.dot(hidden, drop[layer], preferred_element_type=F32).astype(BF16)
        for column in columns:
            send(branch.at[layer, b, cb], branch.at[layer, b, cb], br_ssem.at[layer, b], br_rsem.at[layer, b], (ra, column))

    def finish(layer, b, current, scale):
        arrived(branch.at[layer, b, pl.ds(0, CB - 1)], br_rsem.at[layer, b])
        total = branch[layer, b, 0].astype(F32)
        for i in range(1, CB):
            total += branch[layer, b, i].astype(F32)
        return (residual_scale * current + scale * total).astype(BF16)

    loads[0].wait()
    loads[1].wait()
    span = [slice(b * size, (b + 1) * size) for b in range(BLOCKS)]
    current = [stream[s].astype(F32) for s in span]
    loads[2].wait()
    for b in range(BLOCKS):
        multiply_in(0, b, current[b])
    pl.semaphore_wait(barrier, RA - 1 + CB - 1)
    for b in range(BLOCKS):
        scatter(0, b)
    send_squares(0, jnp.concatenate(current, axis=0))
    for layer in range(2):
        for b in range(BLOCKS):
            activate(layer, b)
        scale = token_scale(layer)
        loads[3 + 3 * layer].wait()
        for b in range(BLOCKS):
            multiply_out(layer, b)
        if layer == 0:
            loads[4].wait()
            loads[5].wait()
        after = []
        for b in range(BLOCKS):
            block = finish(layer, b, current[b], scale[span[b]])
            if layer == 0:
                after.append(block.astype(F32))
                multiply_in(1, b, after[b])
                scatter(1, b)
            else:
                out_ref[span[b]] = block
        if layer == 0:
            send_squares(1, jnp.concatenate(after, axis=0))
            current = after

    for layer in range(2):
        for b in range(BLOCKS):
            arrived(part_in.at[layer, b], part_ssem.at[layer, b])
            arrived(hid.at[layer, b, pl.ds(0, RA - 1)], hid_ssem.at[layer, b])
            arrived(branch.at[layer, b, pl.ds(0, CB - 1)], br_ssem.at[layer, b])
        arrived(sq_in.at[layer], sq_ssem.at[layer])


def per_device(stream, gain_first, lift_first, drop_first, gain_second, lift_second, drop_second):
    tokens, width = stream.shape
    hidden = lift_first.shape[1]
    size = tokens // BLOCKS
    rows = size // SPLIT
    any_spec = pl.BlockSpec(memory_space=pl.ANY)
    dma = pltpu.SemaphoreType.DMA
    return pl.pallas_call(
        kernel,
        out_shape=pltpu.VMEM((tokens, width), BF16),
        in_specs=[any_spec] * 7,
        out_specs=pl.BlockSpec(memory_space=pltpu.VMEM),
        scratch_shapes=[
            pltpu.VMEM((tokens, width), BF16),
            pltpu.VMEM((2, 1, width), F32),
            pltpu.VMEM((2, width, hidden), BF16),
            pltpu.VMEM((2, hidden, width), BF16),
            pltpu.VMEM((2, BLOCKS, RA, rows, LANES), BF16),
            pltpu.VMEM((2, BLOCKS, RA - 1, rows, LANES), BF16),
            pltpu.VMEM((2, BLOCKS, RA, rows, LANES), BF16),
            pltpu.VMEM((2, BLOCKS, CB, size, width), BF16),
            pltpu.VMEM((2, 1, tokens), F32),
            pltpu.VMEM((2, RA - 1, 1, tokens), F32),
            dma((7,)),
            dma((2, BLOCKS)), dma((2, BLOCKS)),
            dma((2, BLOCKS)), dma((2, BLOCKS)),
            dma((2, BLOCKS)), dma((2, BLOCKS)),
            dma((2,)), dma((2,)),
        ],
        compiler_params=pltpu.CompilerParams(collective_id=0, has_side_effects=True),
        name="ffn_pair",
    )(
        stream, gain_first.reshape(1, width), lift_first, drop_first,
        gain_second.reshape(1, width), lift_second, drop_second,
    )


def solution(mesh):
    in_specs = (P(None, "ra"), P("ra"), P("ra", "cb"), P("cb", "ra"), P("ra"), P("ra", "cb"), P("cb", "ra"))
    return jax.shard_map(
        per_device, mesh=mesh, in_specs=in_specs, out_specs=P(None, "ra"), check_vma=False
    )
```

```python
import jax
import jax.numpy as jnp
from jax import lax
from jax.experimental import pallas as pl
from jax.experimental.pallas import tpu as pltpu
from jax.sharding import PartitionSpec as P

MESH = pl.DeviceIdType.MESH
F32 = jnp.float32
BF16 = jnp.bfloat16

residual_scale = 0.25
epsilon = 1e-06

SIDE = 4
RA = SIDE * SIDE
CB = 2 * SIDE
FEATURES = 2048
LANES = 128
BLOCKS = 4
SPLIT = 2
GROUPS = RA // SPLIT

OFFSETS = sorted(
    [(dz, dx) for dz in range(SIDE) for dx in range(SIDE) if (dz, dx) != (0, 0)],
    key=lambda o: -(min(o[0], SIDE - o[0]) + min(o[1], SIDE - o[1])),
)
COLUMN_OFFSETS = [(2, 0), (2, 1), (1, 0), (1, 1), (3, 0), (3, 1), (0, 1)]


def kernel(
    stream_hbm, gain1_hbm, lift1_hbm, drop1_hbm, gain2_hbm, lift2_hbm, drop2_hbm, out_ref,
    stream, gain, lift, drop, part, part_in, hid, branch, sq, sq_in,
    load_sem, part_ssem, part_rsem, hid_ssem, hid_rsem, br_ssem, br_rsem, sq_ssem, sq_rsem,
):
    ra = lax.axis_index("ra")
    cb = lax.axis_index("cb")
    z, x = ra // SIDE, ra % SIDE
    y, core = cb // 2, cb % 2
    tokens = stream.shape[0]
    size = tokens // BLOCKS
    rows = size // SPLIT

    peers = [lax.rem(z + dz, SIDE) * SIDE + lax.rem(x + dx, SIDE) for dz, dx in OFFSETS]
    columns = [lax.rem(y + dy, SIDE) * 2 + lax.rem(core + dc, 2) for dy, dc in COLUMN_OFFSETS]

    barrier = pltpu.get_barrier_semaphore()
    for peer in peers:
        pl.semaphore_signal(barrier, inc=1, device_id=(peer, cb), device_id_type=MESH)
    for column in columns:
        pl.semaphore_signal(barrier, inc=1, device_id=(ra, column), device_id_type=MESH)

    loads = [
        pltpu.make_async_copy(src, dst, load_sem.at[i])
        for i, (src, dst) in enumerate([
            (stream_hbm, stream), (gain1_hbm, gain.at[0]), (lift1_hbm, lift.at[0]), (drop1_hbm, drop.at[0]),
            (gain2_hbm, gain.at[1]), (lift2_hbm, lift.at[1]), (drop2_hbm, drop.at[1]),
        ])
    ]
    for load in loads:
        load.start()

    def send(src, dst, ssem, rsem, device):
        pltpu.make_async_remote_copy(
            src_ref=src, dst_ref=dst, send_sem=ssem, recv_sem=rsem, device_id=device, device_id_type=MESH
        ).start()

    def arrived(ref, rsem):
        pltpu.make_async_copy(ref, ref, rsem).wait()

    def multiply_in(layer, b, current):
        gained = (current * gain[layer]).astype(BF16)
        products = jnp.dot(gained, lift[layer], preferred_element_type=F32).astype(BF16)
        for i in range(RA):
            r, c = i // GROUPS, i % GROUPS
            part[layer, b, i] = products[r * rows:(r + 1) * rows, c * LANES:(c + 1) * LANES]

    def scatter(layer, b):
        for k, peer in enumerate(peers):
            send(part.at[layer, b, peer], part_in.at[layer, b, k], part_ssem.at[layer, b], part_rsem.at[layer, b], (peer, cb))

    def send_squares(layer, current):
        sq[layer] = jnp.sum((current * current).T, axis=0, keepdims=True)
        for k, peer in enumerate(peers):
            send(sq.at[layer], sq_in.at[layer, k], sq_ssem.at[layer], sq_rsem.at[layer], (peer, cb))

    def activate(layer, b):
        arrived(part_in.at[layer, b], part_rsem.at[layer, b])
        total = part[layer, b, ra].astype(F32)
        for k in range(RA - 1):
            total += part_in[layer, b, k].astype(F32)
        positive = jnp.maximum(total, 0.0)
        hid[layer, b, ra] = (positive * positive).astype(BF16)
        for peer in peers:
            send(hid.at[layer, b, ra], hid.at[layer, b, ra], hid_ssem.at[layer, b], hid_rsem.at[layer, b], (peer, cb))

    def token_scale(layer):
        arrived(sq_in.at[layer], sq_rsem.at[layer])
        sums = sq[layer]
        for k in range(RA - 1):
            sums += sq_in[layer, k]
        return jnp.broadcast_to(1.0 / (sums / FEATURES + epsilon), (tokens, tokens)).T

    def multiply_out(layer, b):
        arrived(hid.at[layer, b, pl.ds(0, RA - 1)], hid_rsem.at[layer, b])
        hidden = jnp.concatenate([
            jnp.concatenate([hid[layer, b, r * GROUPS + c] for c in range(GROUPS)], axis=1) for r in range(SPLIT)
        ], axis=0)
        branch[layer, b, cb] = jnp.dot(hidden, drop[layer], preferred_element_type=F32).astype(BF16)
        for column in columns:
            send(branch.at[layer, b, cb], branch.at[layer, b, cb], br_ssem.at[layer, b], br_rsem.at[layer, b], (ra, column))

    def finish(layer, b, current, scale):
        arrived(branch.at[layer, b, pl.ds(0, CB - 1)], br_rsem.at[layer, b])
        total = branch[layer, b, 0].astype(F32)
        for i in range(1, CB):
            total += branch[layer, b, i].astype(F32)
        return (residual_scale * current + scale * total).astype(BF16)

    loads[0].wait()
    loads[1].wait()
    span = [slice(b * size, (b + 1) * size) for b in range(BLOCKS)]
    current = [stream[s].astype(F32) for s in span]
    loads[2].wait()
    for b in range(BLOCKS):
        multiply_in(0, b, current[b])
    pl.semaphore_wait(barrier, RA - 1 + CB - 1)
    for b in range(BLOCKS):
        scatter(0, b)
    send_squares(0, jnp.concatenate(current, axis=0))
    for layer in range(2):
        for b in range(BLOCKS):
            activate(layer, b)
        scale = token_scale(layer)
        loads[3 + 3 * layer].wait()
        for b in range(BLOCKS):
            multiply_out(layer, b)
        if layer == 0:
            loads[4].wait()
            loads[5].wait()
        after = []
        for b in range(BLOCKS):
            block = finish(layer, b, current[b], scale[span[b]])
            if layer == 0:
                after.append(block.astype(F32))
                multiply_in(1, b, after[b])
                scatter(1, b)
            else:
                out_ref[span[b]] = block
        if layer == 0:
            send_squares(1, jnp.concatenate(after, axis=0))
            current = after

    for layer in range(2):
        for b in range(BLOCKS):
            arrived(part_in.at[layer, b], part_ssem.at[layer, b])
            arrived(hid.at[layer, b, pl.ds(0, RA - 1)], hid_ssem.at[layer, b])
            arrived(branch.at[layer, b, pl.ds(0, CB - 1)], br_ssem.at[layer, b])
        arrived(sq_in.at[layer], sq_ssem.at[layer])


def per_device(stream, gain_first, lift_first, drop_first, gain_second, lift_second, drop_second):
    tokens, width = stream.shape
    hidden = lift_first.shape[1]
    size = tokens // BLOCKS
    rows = size // SPLIT
    any_spec = pl.BlockSpec(memory_space=pl.ANY)
    dma = pltpu.SemaphoreType.DMA
    return pl.pallas_call(
        kernel,
        out_shape=pltpu.VMEM((tokens, width), BF16),
        in_specs=[any_spec] * 7,
        out_specs=pl.BlockSpec(memory_space=pltpu.VMEM),
        scratch_shapes=[
            pltpu.VMEM((tokens, width), BF16),
            pltpu.VMEM((2, 1, width), F32),
            pltpu.VMEM((2, width, hidden), BF16),
            pltpu.VMEM((2, hidden, width), BF16),
            pltpu.VMEM((2, BLOCKS, RA, rows, LANES), BF16),
            pltpu.VMEM((2, BLOCKS, RA - 1, rows, LANES), BF16),
            pltpu.VMEM((2, BLOCKS, RA, rows, LANES), BF16),
            pltpu.VMEM((2, BLOCKS, CB, size, width), BF16),
            pltpu.VMEM((2, 1, tokens), F32),
            pltpu.VMEM((2, RA - 1, 1, tokens), F32),
            dma((7,)),
            dma((2, BLOCKS)), dma((2, BLOCKS)),
            dma((2, BLOCKS)), dma((2, BLOCKS)),
            dma((2, BLOCKS)), dma((2, BLOCKS)),
            dma((2,)), dma((2,)),
        ],
        compiler_params=pltpu.CompilerParams(collective_id=0, has_side_effects=True),
        name="ffn_pair",
    )(
        stream, gain_first.reshape(1, width), lift_first, drop_first,
        gain_second.reshape(1, width), lift_second, drop_second,
    )


def solution(mesh):
    in_specs = (P(None, "ra"), P("ra"), P("ra", "cb"), P("cb", "ra"), P("ra"), P("ra", "cb"), P("cb", "ra"))
    return jax.shard_map(
        per_device, mesh=mesh, in_specs=in_specs, out_specs=P(None, "ra"), check_vma=False
    )
```
